256 devices in a mesh: fs: 64 (over z, x, core), tp: 4 (over y).
Axes of the slice: x: 4, y: 4, z: 8, core: 2. Of those that a mesh axis runs over, the one named last changes fastest.
Arguments:
- inputs: bfloat16 [65536, 4096], P('fs'), may hold values from -16 to 16
- key_cot: bfloat16 [65536, 2048], P('fs', 'tp'), may hold values from -0.0014648438 to 0.0014648438
- value_cot: bfloat16 [65536, 4096], P('fs', 'tp'), may hold values from -0.0014648438 to 0.0014648438
- key_basis: bfloat16 [4096, 256], P('fs'), may hold values from -3.125 to 3.125, as said below
- value_basis: bfloat16 [4096, 256], P('fs'), may hold values from -3.125 to 3.125, as said below
- key_weight: float32 [4096, 2048], P('fs', 'tp'), may hold values from -3 to 3
- value_weight: float32 [4096, 4096], P('fs', 'tp'), may hold values from -3 to 3
- key_mean: float32 [256, 2048], P('fs', 'tp'), may hold values from -6 to 6
- key_var: float32 [256, 2048], P('fs', 'tp'), may hold values from 0.02 to 2
- value_mean: float32 [256, 4096], P('fs', 'tp'), may hold values from -6 to 6
- value_var: float32 [256, 4096], P('fs', 'tp'), may hold values from 0.02 to 2
Outputs:
- key_weight_new: float32 [4096, 2048], P('fs', 'tp')
- value_weight_new: float32 [4096, 4096], P('fs', 'tp')
- key_copy: bfloat16 [4096, 2048], P('fs', 'tp')
- value_copy: bfloat16 [4096, 4096], P('fs', 'tp')
- key_mean_new: float32 [256, 2048], P('fs', 'tp')
- key_var_new: float32 [256, 2048], P('fs', 'tp')
- value_mean_new: float32 [256, 4096], P('fs', 'tp')
- value_var_new: float32 [256, 4096], P('fs', 'tp')
The draws below stay inside these ranges and needn't reach their ends.
Inputs may be any that keep to these rules, and one draw needn't show every extreme that they name: `key_basis`: real-valued factors of full rank. `value_basis`: real-valued factors of full rank.
All inputs are finite; a program needn't handle non-finite values.
Results may differ from the reference program's by a relative error of at most 0.0045.
Values may be sent and summed in bfloat16 or wider, within the bound.
No kernel may reach another device: no remote copies, remote signals or barrier semaphores. Data moves between devices by JAX's collectives and lax.ppermute only.
A program may use at most 64 MiB of HBM per device.

```python
import math
import jax
import jax.numpy as jnp
from jax import lax

D = 4096
RANK = 256
TOK_DEV = 1024
TOKENS = 65536
QK = 2048
VW = 4096
N_FS = 64


def factor_draw(key):
    row_pos = jnp.arange(D, dtype=jnp.float32)[:, None] / D
    jitter = jax.random.uniform(jax.random.fold_in(key, 11), (D, 1), jnp.float32)
    row_scale = jnp.exp(jnp.log(10.0) * (0.5 * row_pos + 0.5 * jitter))
    entries = jnp.clip(jax.random.normal(jax.random.fold_in(key, 12), (D, RANK), jnp.float32), -5.0, 5.0)
    return (entries * row_scale * RANK ** (-0.5)).astype(jnp.bfloat16)


def draw_key_basis(key, part):
    return factor_draw(jax.random.fold_in(key, 21))


def draw_value_basis(key, part):
    return factor_draw(jax.random.fold_in(key, 22))


def spiked(result, key, source, target, shards_of, factor):
    owner, partner = [(jnp.arange(result.shape[dim]) // (result.shape[dim] // shards_of)).reshape([-1 if axis == dim else 1 for axis in range(result.ndim)]) for dim in (source, target)]
    chosen = jax.random.permutation(key, shards_of)[partner]
    strong = (owner == chosen) | (owner == (partner + shards_of // 2) % shards_of)
    return jnp.where(strong, factor * result, result)


def block_levels(key, extent, cuts, low, high):
    def one(axis_at, parts):
        heights = jax.random.uniform(jax.random.fold_in(jax.random.fold_in(key, 6), axis_at), (parts,), jnp.float32, low / len(cuts), high / len(cuts))
        return jnp.repeat(jnp.exp(heights), extent[axis_at] // parts).reshape((-1,) + (1,) * (len(extent) - axis_at - 1))

    factor_of = one(*cuts[0])
    for cut in cuts[1:]:
        factor_of = factor_of * one(*cut)
    return factor_of


def centred(own_key, extent, spread, limit, pieces=(), kind=jnp.bfloat16):
    gain = block_levels(own_key, extent, pieces, -0.22, 0.18) if pieces else 1.0
    values = jax.random.normal(own_key, extent, jnp.float32) * spread * gain
    return jnp.minimum(jnp.maximum(values, -limit), limit).astype(kind)


def noise_with(stream_key, shape, deviation, reach, cuts, heavy, kind=jnp.bfloat16):
    values = deviation * jax.random.normal(stream_key, shape, jnp.float32)
    if cuts:
        values = values * block_levels(stream_key, shape, cuts, -0.22, 0.18)
    return jnp.clip(spiked(values, jax.random.fold_in(stream_key, 3), *heavy), -reach, reach).astype(kind)


def setup_inputs(seed: int = 0) -> dict:
    streams_of = jax.random.split(jax.random.key(seed), 12)
    return {
        "inputs": noise_with(streams_of[0], (TOKENS, D), 1.0, 16.0, ((0, 64),), (0, 1, 64, 4.0)),
        "key_cot": centred(streams_of[1], (TOKENS, QK), (0.25 * RANK ** 0.5 * (D * TOK_DEV * N_FS) ** -0.5), 0.0014648438, ((0, 64), (1, 4))),
        "value_cot": centred(streams_of[2], (TOKENS, VW), (0.25 * RANK ** 0.5 * (D * TOK_DEV * N_FS) ** -0.5), 0.0014648438, ((0, 64), (1, 4))),
        "key_basis": draw_key_basis(jax.random.fold_in(streams_of[11], 71), 0),
        "value_basis": draw_value_basis(jax.random.fold_in(streams_of[11], 71), 0),
        "key_weight": centred(streams_of[5], (D, QK), 0.5, 3.0, ((0, 64), (1, 4)), jnp.float32),
        "value_weight": centred(streams_of[6], (D, VW), 0.5, 3.0, ((0, 64), (1, 4)), jnp.float32),
        "key_mean": centred(streams_of[7], (RANK, QK), 1.0, 6.0, ((0, 64), (1, 4)), jnp.float32),
        "key_var": jnp.clip(jnp.exp(math.log(2.0) - 4.6051702 * jax.random.uniform(streams_of[8], (RANK, QK), jnp.float32) ** block_levels(streams_of[8], (RANK, QK), ((0, 64), (1, 4)), -0.2, 0.2)), 0.02, 2.0),
        "value_mean": centred(streams_of[9], (RANK, VW), 1.0, 6.0, ((0, 64), (1, 4)), jnp.float32),
        "value_var": jnp.clip(jnp.exp(math.log(2.0) - 4.6051702 * jax.random.uniform(streams_of[10], (RANK, VW), jnp.float32) ** block_levels(streams_of[10], (RANK, VW), ((0, 64), (1, 4)), -0.2, 0.2)), 0.02, 2.0),
    }


def moment_update(inputs, cot, basis, mean, var):
    grad = jnp.dot(inputs.T, cot, preferred_element_type=jnp.float32)
    basis_wide = basis.astype(jnp.float32)
    proj = jnp.dot(basis_wide.T, grad, precision=lax.Precision.HIGHEST)
    mean_new = 0.8 * mean + 0.2 * proj
    var_new = 0.9 * var + 0.1 * proj * proj
    direction = mean_new / (jnp.sqrt(var_new) + 1e-08)
    update = jnp.dot(basis_wide, direction, precision=lax.Precision.HIGHEST)
    return (update, mean_new, var_new)

def apply_step(weight, update):
    factor = jnp.minimum(1.0, 0.5 * lax.rsqrt(jnp.mean(update * update) + 1e-06))
    weight_new = weight - 0.25 * factor * update
    return (weight_new, weight_new.astype(jnp.bfloat16))

def reference(inputs, key_cot, value_cot, key_basis, value_basis, key_weight, value_weight, key_mean, key_var, value_mean, value_var):
    key_update, key_mean_new, key_var_new = moment_update(inputs, key_cot, key_basis, key_mean, key_var)
    value_update, value_mean_new, value_var_new = moment_update(inputs, value_cot, value_basis, value_mean, value_var)
    key_weight_new, key_copy = apply_step(key_weight, key_update)
    value_weight_new, value_copy = apply_step(value_weight, value_update)
    return (key_weight_new, value_weight_new, key_copy, value_copy, key_mean_new, key_var_new, value_mean_new, value_var_new)
```

```python
import jax
import jax.numpy as jnp
from jax import lax
from jax.sharding import Mesh
from jax.sharding import PartitionSpec as P

FS = ("z", "x", "c")
PLANE = ("z", "x")
SWAP = [(0, 1), (1, 0)]
BF = jnp.bfloat16
F32 = jnp.float32


def spread(shard, axes):
    peers = lax.axis_size(axes)
    return lax.all_to_all(
        jnp.broadcast_to(shard[None], (peers, *shard.shape)), axes, 0, 0, tiled=True
    )


def other_core(a):
    return lax.ppermute(a, "c", SWAP)


def in_core_order(c, own, other):
    return jnp.where(c == 0, own, other), jnp.where(c == 0, other, own)


def half(a, which):
    w = a.shape[1] // 2
    return lax.dynamic_slice_in_dim(a, which * w, w, axis=1)


def halves(k, v, which):
    return jnp.concatenate([half(k, which), half(v, which)], axis=1)


def full_cols(c, own, other):
    first, second = in_core_order(c, own, other)
    n = first.shape[1] // 3
    k = jnp.concatenate([first[:, :n], second[:, :n]], axis=1)
    v = jnp.concatenate([first[:, n:], second[:, n:]], axis=1)
    return k, v


def shards(
    inputs,
    key_cot,
    value_cot,
    key_basis,
    value_basis,
    key_weight,
    value_weight,
    key_mean,
    key_var,
    value_mean,
    value_var,
):
    c = lax.axis_index("c")
    t = lax.axis_index("tp")
    planes = lax.axis_size(PLANE)
    tp_size = lax.axis_size("tp")
    fs_size = lax.axis_size(FS)

    stats_out = jnp.concatenate(
        [halves(key_mean, value_mean, 1 - c), halves(key_var, value_var, 1 - c)], axis=0
    )
    stats_in = other_core(stats_out)
    rows = key_mean.shape[0]
    mean8 = jnp.concatenate(
        in_core_order(c, halves(key_mean, value_mean, c), stats_in[:rows]), axis=0
    )
    var8 = jnp.concatenate(
        in_core_order(c, halves(key_var, value_var, c), stats_in[rows:]), axis=0
    )

    both = jnp.concatenate([key_basis, value_basis], axis=1)
    quarter = both.shape[1] // tp_size
    mine = lax.dynamic_slice_in_dim(both, t * quarter, quarter, axis=1)
    own = spread(mine, PLANE)
    other = other_core(own)
    basis = jnp.stack(in_core_order(c, own, other), axis=1).reshape(-1, quarter)
    mapped = lax.dot_general(
        basis, inputs, (((0,), (1,)), ((), ())), preferred_element_type=F32
    ).astype(BF)
    mapped = spread(mapped, "tp").reshape(-1, inputs.shape[0])
    rank = mapped.shape[0] // 2
    key_part = jnp.dot(mapped[:rank], key_cot, preferred_element_type=F32)
    value_part = jnp.dot(mapped[rank:], value_cot, preferred_element_type=F32)

    got = other_core(halves(key_part, value_part, 1 - c).astype(BF))
    pair = (halves(key_part, value_part, c) + got.astype(F32)).astype(BF)
    width = pair.shape[1]
    arrived = lax.all_to_all(pair.reshape(planes, -1, width), PLANE, 0, 0, tiled=True)
    proj = jnp.sum(arrived.astype(F32), axis=0)
    mean_new = 0.8 * mean8 + 0.2 * proj
    var_new = 0.9 * var8 + 0.1 * proj * proj
    direction = (mean_new / (jnp.sqrt(var_new) + 1e-08)).astype(BF)

    own_dir = spread(direction, PLANE).reshape(rank, width)
    def my_rows(a, which):
        return lax.dynamic_slice_in_dim(a, which * rows, rows, axis=0)

    back_out = jnp.concatenate([my_rows(mean_new, 1 - c), my_rows(var_new, 1 - c)], axis=0)
    back = other_core(back_out)
    key_mean_new, value_mean_new = full_cols(c, my_rows(mean_new, c), back[:rows])
    key_var_new, value_var_new = full_cols(c, my_rows(var_new, c), back[rows:])

    key_dir, value_dir = full_cols(c, own_dir, other_core(own_dir))
    key_update = jnp.dot(key_basis, key_dir, preferred_element_type=F32)
    value_update = jnp.dot(value_basis, value_dir, preferred_element_type=F32)
    sq = jnp.stack([jnp.sum(key_update * key_update), jnp.sum(value_update * value_update)])
    sq = jnp.sum(spread(sq[None], ("c", "tp")), axis=0)
    sq = jnp.sum(spread(sq, PLANE), axis=0)[0]

    key_count = float(key_weight.size * fs_size * tp_size)
    value_count = float(value_weight.size * fs_size * tp_size)
    key_factor = jnp.minimum(1.0, 0.5 * lax.rsqrt(sq[0] / key_count + 1e-06))
    value_factor = jnp.minimum(1.0, 0.5 * lax.rsqrt(sq[1] / value_count + 1e-06))
    key_weight_new = key_weight - 0.25 * key_factor * key_update
    value_weight_new = value_weight - 0.25 * value_factor * value_update
    return (
        key_weight_new,
        value_weight_new,
        key_weight_new.astype(BF),
        value_weight_new.astype(BF),
        key_mean_new,
        key_var_new,
        value_mean_new,
        value_var_new,
    )


def solution(mesh):
    split = Mesh(mesh.devices.reshape(8, 4, 2, mesh.shape["tp"]), ("z", "x", "c", "tp"))
    rows, tiles = P(FS, None), P(FS, "tp")
    return jax.shard_map(
        shards,
        mesh=split,
        in_specs=(rows, tiles, tiles, rows, rows) + (tiles,) * 6,
        out_specs=(tiles,) * 8,
        check_vma=False,
    )
```

```python
import functools

import jax
import jax.numpy as jnp
from jax import lax
from jax.experimental import pallas as pl
from jax.experimental.pallas import tpu as pltpu
from jax.sharding import Mesh
from jax.sharding import PartitionSpec as P


FS = ("z", "x", "c")
PLANE = ("z", "x")
SWAP = [(0, 1), (1, 0)]
BF = jnp.bfloat16
F32 = jnp.float32
VMEM = pl.BlockSpec(memory_space=pltpu.VMEM)


def spread(shard, axes):
    peers = lax.axis_size(axes)
    return lax.all_to_all(
        jnp.broadcast_to(shard[None], (peers, *shard.shape)), axes, 0, 0, tiled=True
    )


def other_core(a):
    return lax.ppermute(a, "c", SWAP)


def shape(dims, dtype=F32):
    return jax.ShapeDtypeStruct(dims, dtype)


def local(body, outs, flops=0, mib=16):
    def call(*arrays):
        return pl.pallas_call(
            body,
            out_shape=outs,
            in_specs=[VMEM] * len(arrays),
            out_specs=(VMEM,) * len(outs) if isinstance(outs, tuple) else VMEM,
            compiler_params=pltpu.CompilerParams(vmem_limit_bytes=mib << 20),
            cost_estimate=pl.CostEstimate(
                flops=max(flops, 1 << 20), bytes_accessed=1 << 20, transcendentals=0
            ),
        )(*arrays)

    return call


BLOCKS = 8


def mapped_body(x_ref, own_ref, other_ref, out_ref, held, basis, sems):
    block = held.shape[1]

    def load(i):
        return pltpu.make_async_copy(
            x_ref.at[pl.ds(i * block, block)], held.at[i], sems.at[i]
        )

    for i in range(BLOCKS):
        load(i).start()
    first = lax.axis_index("c") == 0
    own, other = own_ref[...], other_ref[...]
    basis[:, 0] = jnp.where(first, own, other)
    basis[:, 1] = jnp.where(first, other, own)
    whole = basis[...].reshape(x_ref.shape[1], -1)
    for i in range(BLOCKS):
        load(i).wait()
        m = jnp.dot(held[i], whole, preferred_element_type=F32).T.astype(BF)
        for k in range(out_ref.shape[0]):
            out_ref[k, :, i * block : (i + 1) * block] = m


def mapped_kernel(inputs, own, other, tp_size):
    tok, depth = inputs.shape
    planes, rows, quarter = own.shape
    return pl.pallas_call(
        mapped_body,
        out_shape=shape((tp_size, quarter, tok), BF),
        in_specs=[pl.BlockSpec(memory_space=pltpu.HBM), VMEM, VMEM],
        out_specs=VMEM,
        scratch_shapes=[
            pltpu.VMEM((BLOCKS, tok // BLOCKS, depth), BF),
            pltpu.VMEM((planes, 2, rows, quarter), BF),
            pltpu.SemaphoreType.DMA((BLOCKS,)),
        ],
        name="mapped",
        compiler_params=pltpu.CompilerParams(vmem_limit_bytes=48 << 20),
        cost_estimate=pl.CostEstimate(
            flops=4 * tok * depth * quarter, bytes_accessed=2 * tok * depth, transcendentals=0
        ),
    )(inputs, own, other)


def part_body(mine, m_ref, k_ref, v_ref, out_ref):
    c = lax.axis_index("c")
    side = c if mine else 1 - c
    rank = m_ref.shape[0] // 2
    kw, vw = k_ref.shape[1] // 2, v_ref.shape[1] // 2
    kc = k_ref[:, pl.ds(pl.multiple_of(side * kw, 128), kw)]
    vc = v_ref[:, pl.ds(pl.multiple_of(side * vw, 128), vw)]
    out_ref[:, :kw] = jnp.dot(m_ref[:rank], kc, preferred_element_type=F32).astype(out_ref.dtype)
    out_ref[:, kw:] = jnp.dot(m_ref[rank:], vc, preferred_element_type=F32).astype(out_ref.dtype)


def stats_body(km, kv, vm, vv, kb, vb, mine, theirs, rows_kb, rows_vb):
    c = lax.axis_index("c")
    rows = km.shape[0]
    kw, vw = km.shape[1] // 2, vm.shape[1] // 2
    for out, side in ((mine, c), (theirs, 1 - c)):
        ks, vs = (pl.ds(pl.multiple_of(side * w, 128), w) for w in (kw, vw))
        out[:rows, :kw] = km[:, ks]
        out[:rows, kw:] = vm[:, vs]
        out[rows:, :kw] = kv[:, ks]
        out[rows:, kw:] = vv[:, vs]
    rows_kb[...] = kb[...]
    rows_vb[...] = vb[...]


def moments_body(arrived, mine, theirs, dirs, own_new, back):
    first = lax.axis_index("c") == 0
    rows = mine.shape[0] // 2
    proj = jnp.sum(arrived[...].astype(F32), axis=0)

    def both(at):
        own, other = mine[at : at + rows], theirs[at : at + rows]
        low = jnp.where(first, own, other)
        high = jnp.where(first, other, own)
        return jnp.concatenate([low, high], axis=0)

    mean_new = 0.8 * both(0) + 0.2 * proj
    var_new = 0.9 * both(rows) + 0.1 * proj * proj
    d = (mean_new / (jnp.sqrt(var_new) + 1e-08)).astype(BF)
    dirs[...] = jnp.broadcast_to(d[None], dirs.shape)
    for at, new in ((0, mean_new), (rows, var_new)):
        low, high = new[:rows], new[rows:]
        own_new[at : at + rows] = jnp.where(first, low, high)
        back[at : at + rows] = jnp.where(first, high, low)


def placed_body(own, back, km, kv, vm, vv):
    c = lax.axis_index("c")
    rows = km.shape[0]
    kw, vw = km.shape[1] // 2, vm.shape[1] // 2
    for src, side in ((own, c), (back, 1 - c)):
        ks, vs = (pl.ds(pl.multiple_of(side * w, 128), w) for w in (kw, vw))
        km[:, ks] = src[:rows, :kw]
        vm[:, vs] = src[:rows, kw:]
        kv[:, ks] = src[rows:, :kw]
        vv[:, vs] = src[rows:, kw:]


def gram_body(own, other, own_y, other_y, out):
    first = lax.axis_index("tp") % 2 == 0
    mine = jnp.concatenate([own[...], other[...]], axis=0)
    theirs = jnp.concatenate([own_y[...], other_y[...]], axis=0)
    low = jnp.where(first, mine, theirs)
    high = jnp.where(first, theirs, mine)
    cols = jnp.concatenate([low, high], axis=1)
    out[...] = lax.dot_general(
        cols, cols, (((0,), (0,)), ((), ())), preferred_element_type=F32
    )


def update_body(own, other, kb, vb, gram, gram_y, key_up, value_up, sums):
    c, t = lax.axis_index("c"), lax.axis_index("tp")
    kw, vw = key_up.shape[1] // 2, value_up.shape[1] // 2
    is_key = t < 2
    key_gram = jnp.where(is_key, gram[...], gram_y[...])
    value_gram = jnp.where(is_key, gram_y[...], gram[...])

    def pieces(g):
        a = g.astype(BF)
        r = g - a.astype(F32)
        b = r.astype(BF)
        return a, b, (r - b.astype(F32)).astype(BF)

    def square(ps, d):
        gd = sum(jnp.dot(p, d, preferred_element_type=F32) for p in ps)
        return jnp.sum(gd * d.astype(F32), axis=0, keepdims=True)

    kp, vp = pieces(key_gram), pieces(value_gram)
    ksq = jnp.zeros((1, kw), F32)
    vsq = jnp.zeros((1, vw), F32)
    for src, side in ((own, c), (other, 1 - c)):
        dk, dv = src[:, :kw], src[:, kw:]
        ks, vs = (pl.ds(pl.multiple_of(side * w, 128), w) for w in (kw, vw))
        key_up[:, ks] = jnp.dot(kb[...], dk, preferred_element_type=F32)
        value_up[:, vs] = jnp.dot(vb[...], dv, preferred_element_type=F32)
        ksq += square(kp, dk)
        vsq += square(vp, dv)
    lane = lax.broadcasted_iota(jnp.int32, sums.shape, 1)
    sums[...] = jnp.where(lane == 0, jnp.sum(ksq), jnp.where(lane == 1, jnp.sum(vsq), 0.0))


def finish_body(counts, s0, s1, s2, s3, ku, vu, kw, vw, kn, vn, kc, vc):
    total = (s0[...] + s1[...]) + (s2[...] + s3[...])
    for lane, u, w, n, b in ((0, ku, kw, kn, kc), (1, vu, vw, vn, vc)):
        mean = total[:, lane : lane + 1] / counts[lane]
        factor = jnp.minimum(1.0, 0.5 * lax.rsqrt(mean + 1e-06))
        new = w[...] - 0.25 * factor * u[...]
        n[...] = new
        b[...] = new.astype(BF)


def step(
    inputs,
    key_cot,
    value_cot,
    key_basis,
    value_basis,
    key_weight,
    value_weight,
    key_mean,
    key_var,
    value_mean,
    value_var,
):
    t = lax.axis_index("tp")
    planes = lax.axis_size(PLANE)
    tp_size = lax.axis_size("tp")
    devices = lax.axis_size(FS) * tp_size
    moments = (key_mean, key_var, value_mean, value_var)
    rank = key_basis.shape[1]
    width = (key_cot.shape[1] + value_cot.shape[1]) // 2
    two_rows = 2 * key_mean.shape[0]

    both = jnp.concatenate([key_basis, value_basis], axis=1)
    quarter = both.shape[1] // tp_size
    own = spread(lax.dynamic_slice_in_dim(both, t * quarter, quarter, axis=1), PLANE)
    other = other_core(own)
    mapped = mapped_kernel(inputs, own, other, tp_size)
    mapped = lax.all_to_all(mapped, "tp", 0, 0, tiled=True)
    mapped, own, other = lax.optimization_barrier((mapped, own, other))
    mapped = mapped.reshape(-1, inputs.shape[0])

    flops = mapped.size * 2 * width // 2
    theirs = local(
        functools.partial(part_body, False), shape((rank, width), BF), flops
    )(mapped, key_cot, value_cot)
    got = other_core(theirs)
    ours = local(functools.partial(part_body, True), shape((rank, width)), flops)(
        mapped, key_cot, value_cot
    )
    pair = (ours + got.astype(F32)).astype(BF)

    beside = [(i, i ^ 1) for i in range(tp_size)]
    across = [(i, tp_size - 1 - i) for i in range(tp_size)]
    own_y = lax.ppermute(own, "tp", beside)
    other_y = lax.ppermute(other, "tp", beside)

    stat = shape((two_rows, width))
    mine, theirs, key_rows, value_rows = local(
        stats_body, (stat, stat, shape(key_basis.shape, BF), shape(value_basis.shape, BF))
    )(*moments, key_basis, value_basis)
    stats = other_core(theirs)
    arrived = lax.all_to_all(pair.reshape(planes, -1, width), PLANE, 0, 0, tiled=True)
    dirs, own_new, back = local(
        moments_body, (shape(arrived.shape, BF), stat, stat)
    )(arrived, mine, stats)
    own_dir = lax.all_to_all(dirs, PLANE, 0, 0, tiled=True).reshape(rank, width)

    flat = [a.reshape(-1, quarter) for a in (own, other, own_y, other_y)]
    gram = local(gram_body, shape((rank, rank)), 4 * flat[0].size * rank)(*flat)
    gram_y = lax.ppermute(gram, "tp", across)
    new_moments = local(placed_body, tuple(shape(a.shape) for a in moments))(
        own_new, other_core(back)
    )

    key_up, value_up, sums = local(
        update_body,
        (shape(key_weight.shape), shape(value_weight.shape), shape((1, 128))),
        8 * rank * rank * width,
    )(own_dir, other_core(own_dir), key_rows, value_rows, gram, gram_y)
    sums = [sums] + [
        lax.ppermute(sums, "tp", [(i, (i + k) % tp_size) for i in range(tp_size)])
        for k in range(1, tp_size)
    ]
    counts = (float(key_weight.size * devices), float(value_weight.size * devices))
    key_new, value_new, key_copy, value_copy = local(
        functools.partial(finish_body, counts),
        (
            shape(key_weight.shape),
            shape(value_weight.shape),
            shape(key_weight.shape, BF),
            shape(value_weight.shape, BF),
        ),
    )(*sums, key_up, value_up, key_weight, value_weight)
    key_mean_new, key_var_new, value_mean_new, value_var_new = new_moments
    return (
        key_new,
        value_new,
        key_copy,
        value_copy,
        key_mean_new,
        key_var_new,
        value_mean_new,
        value_var_new,
    )


def solution(mesh):
    split = Mesh(mesh.devices.reshape(8, 4, 2, mesh.shape["tp"]), ("z", "x", "c", "tp"))
    rows, tiles = P(FS, None), P(FS, "tp")
    return jax.shard_map(
        step,
        mesh=split,
        in_specs=(rows, tiles, tiles, rows, rows) + (tiles,) * 6,
        out_specs=(tiles,) * 8,
        check_vma=False,
    )
```

```python
import functools

import jax
import jax.numpy as jnp
from jax import lax
from jax.experimental import pallas as pl
from jax.experimental.pallas import tpu as pltpu
from jax.sharding import Mesh
from jax.sharding import PartitionSpec as P


FS = ("z", "x", "c")
PLANE = ("z", "x")
SWAP = [(0, 1), (1, 0)]
BF = jnp.bfloat16
F32 = jnp.float32
VMEM = pl.BlockSpec(memory_space=pltpu.VMEM)


def spread(shard, axes):
    peers = lax.axis_size(axes)
    return lax.all_to_all(
        jnp.broadcast_to(shard[None], (peers, *shard.shape)), axes, 0, 0, tiled=True
    )


def other_core(a):
    return lax.ppermute(a, "c", SWAP)


def shape(dims, dtype=F32):
    return jax.ShapeDtypeStruct(dims, dtype)


def local(body, outs, flops=0, mib=16):
    def call(*arrays):
        return pl.pallas_call(
            body,
            out_shape=outs,
            in_specs=[VMEM] * len(arrays),
            out_specs=(VMEM,) * len(outs) if isinstance(outs, tuple) else VMEM,
            compiler_params=pltpu.CompilerParams(vmem_limit_bytes=mib << 20),
            cost_estimate=pl.CostEstimate(
                flops=max(flops, 1 << 20), bytes_accessed=1 << 20, transcendentals=0
            ),
        )(*arrays)

    return call


PIECES = 4


def mapped_body(start, fresh, *refs):
    if fresh:
        x_ref, own_ref, other_ref, out_ref, basis, held, sems = refs
    else:
        x_ref, basis, out_ref, held, sems = refs
    tok, piece = held.shape[1:]

    def load(i):
        return pltpu.make_async_copy(
            x_ref.at[pl.ds(start, tok), pl.ds(i * piece, piece)], held.at[i], sems.at[i]
        )

    for i in range(PIECES):
        load(i).start()
    if fresh:
        first = lax.axis_index("c") == 0
        planes, rows, quarter = own_ref.shape
        own, other = own_ref[...], other_ref[...]
        low = jnp.where(first, own, other)
        high = jnp.where(first, other, own)
        basis[...] = jnp.stack([low, high], axis=1).reshape(2 * planes * rows, quarter)
    total = jnp.zeros((tok, out_ref.shape[0]), F32)
    for i in range(PIECES):
        load(i).wait()
        total += jnp.dot(
            held[i], basis[i * piece : (i + 1) * piece], preferred_element_type=F32
        )
    out_ref[...] = total.T.astype(BF)


def mapped_kernel(inputs, start, tok, quarter, *factor):
    depth = inputs.shape[1]
    fresh = len(factor) == 2
    out = shape((quarter, tok), BF)
    return pl.pallas_call(
        functools.partial(mapped_body, start, fresh),
        out_shape=(out, shape((depth, quarter), BF)) if fresh else out,
        in_specs=[pl.BlockSpec(memory_space=pltpu.HBM)] + [VMEM] * len(factor),
        out_specs=(VMEM, VMEM) if fresh else VMEM,
        scratch_shapes=[
            pltpu.VMEM((PIECES, tok, depth // PIECES), BF),
            pltpu.SemaphoreType.DMA((PIECES,)),
        ],
        name="mapped",
        compiler_params=pltpu.CompilerParams(vmem_limit_bytes=48 << 20),
        cost_estimate=pl.CostEstimate(
            flops=4 * tok * depth * quarter, bytes_accessed=2 * tok * depth, transcendentals=0
        ),
    )(inputs, *factor)


def part_half(side, m_ref, k_ref, v_ref, out_ref):
    rank = m_ref.shape[0] // 2
    kw, vw = k_ref.shape[1] // 2, v_ref.shape[1] // 2
    kc = k_ref[:, pl.ds(pl.multiple_of(side * kw, 128), kw)]
    vc = v_ref[:, pl.ds(pl.multiple_of(side * vw, 128), vw)]
    out_ref[:, :kw] = jnp.dot(m_ref[:rank], kc, preferred_element_type=F32).astype(out_ref.dtype)
    out_ref[:, kw:] = jnp.dot(m_ref[rank:], vc, preferred_element_type=F32).astype(out_ref.dtype)


def part_theirs_body(*refs):
    blocks, (k_ref, v_ref, m_ref, out_ref) = refs[:-4], refs[-4:]
    t = lax.axis_index("tp")
    quarter, tok = blocks[0].shape
    peers = len(blocks) // 2
    for away in range(peers):
        rows = pl.ds(pl.multiple_of(lax.rem(t + away, peers) * quarter, quarter), quarter)
        m_ref[rows, :tok] = blocks[2 * away][...]
        m_ref[rows, tok:] = blocks[2 * away + 1][...]
    part_half(1 - lax.axis_index("c"), m_ref, k_ref, v_ref, out_ref)


def part_ours_body(m_ref, k_ref, v_ref, out_ref):
    part_half(lax.axis_index("c"), m_ref, k_ref, v_ref, out_ref)


def stats_body(km, kv, vm, vv, *refs):
    held, (mine, theirs), staged = refs[:4], refs[4:6], refs[6:]
    c = lax.axis_index("c")
    rows = km.shape[0]
    kw, vw = km.shape[1] // 2, vm.shape[1] // 2
    for out, side in ((mine, c), (theirs, 1 - c)):
        ks, vs = (pl.ds(pl.multiple_of(side * w, 128), w) for w in (kw, vw))
        out[:rows, :kw] = km[:, ks]
        out[:rows, kw:] = vm[:, vs]
        out[rows:, :kw] = kv[:, ks]
        out[rows:, kw:] = vv[:, vs]
    for src, dst in zip(held, staged):
        dst[...] = src[...]


def moments_body(arrived, mine, theirs, dirs, own_new, back):
    first = lax.axis_index("c") == 0
    rows = mine.shape[0] // 2
    proj = jnp.sum(arrived[...].astype(F32), axis=0)

    def both(at):
        own, other = mine[at : at + rows], theirs[at : at + rows]
        low = jnp.where(first, own, other)
        high = jnp.where(first, other, own)
        return jnp.concatenate([low, high], axis=0)

    mean_new = 0.8 * both(0) + 0.2 * proj
    var_new = 0.9 * both(rows) + 0.1 * proj * proj
    d = (mean_new / (jnp.sqrt(var_new) + 1e-08)).astype(BF)
    dirs[...] = jnp.broadcast_to(d[None], dirs.shape)
    for at, new in ((0, mean_new), (rows, var_new)):
        low, high = new[:rows], new[rows:]
        own_new[at : at + rows] = jnp.where(first, low, high)
        back[at : at + rows] = jnp.where(first, high, low)


def placed_body(own, back, km, kv, vm, vv):
    c = lax.axis_index("c")
    rows = km.shape[0]
    kw, vw = km.shape[1] // 2, vm.shape[1] // 2
    for src, side in ((own, c), (back, 1 - c)):
        ks, vs = (pl.ds(pl.multiple_of(side * w, 128), w) for w in (kw, vw))
        km[:, ks] = src[:rows, :kw]
        vm[:, vs] = src[:rows, kw:]
        kv[:, ks] = src[rows:, :kw]
        vv[:, vs] = src[rows:, kw:]


def gram_body(mine, beside, out):
    first = lax.axis_index("tp") % 2 == 0
    low = jnp.where(first, mine[...], beside[...])
    high = jnp.where(first, beside[...], mine[...])
    cols = jnp.concatenate([low, high], axis=1)
    out[...] = lax.dot_general(
        cols, cols, (((0,), (0,)), ((), ())), preferred_element_type=F32
    )


def update_body(own, other, kb, vb, gram, gram_y, key_up, value_up, sums):
    c, t = lax.axis_index("c"), lax.axis_index("tp")
    kw, vw = key_up.shape[1] // 2, value_up.shape[1] // 2
    is_key = t < 2
    key_gram = jnp.where(is_key, gram[...], gram_y[...])
    value_gram = jnp.where(is_key, gram_y[...], gram[...])

    def pieces(g):
        a = g.astype(BF)
        r = g - a.astype(F32)
        b = r.astype(BF)
        return a, b, (r - b.astype(F32)).astype(BF)

    def square(ps, d):
        gd = sum(jnp.dot(p, d, preferred_element_type=F32) for p in ps)
        return jnp.sum(gd * d.astype(F32), axis=0, keepdims=True)

    kp, vp = pieces(key_gram), pieces(value_gram)
    ksq = jnp.zeros((1, kw), F32)
    vsq = jnp.zeros((1, vw), F32)
    for src, side in ((own, c), (other, 1 - c)):
        dk, dv = src[:, :kw], src[:, kw:]
        ks, vs = (pl.ds(pl.multiple_of(side * w, 128), w) for w in (kw, vw))
        key_up[:, ks] = jnp.dot(kb[...], dk, preferred_element_type=F32)
        value_up[:, vs] = jnp.dot(vb[...], dv, preferred_element_type=F32)
        ksq += square(kp, dk)
        vsq += square(vp, dv)
    lane = lax.broadcasted_iota(jnp.int32, sums.shape, 1)
    sums[...] = jnp.where(lane == 0, jnp.sum(ksq), jnp.where(lane == 1, jnp.sum(vsq), 0.0))


def finish_body(counts, s0, s1, s2, s3, ku, vu, kw, vw, kn, vn, kc, vc):
    total = (s0[...] + s1[...]) + (s2[...] + s3[...])
    for lane, u, w, n, b in ((0, ku, kw, kn, kc), (1, vu, vw, vn, vc)):
        mean = total[:, lane : lane + 1] / counts[lane]
        factor = jnp.minimum(1.0, 0.5 * lax.rsqrt(mean + 1e-06))
        new = w[...] - 0.25 * factor * u[...]
        n[...] = new
        b[...] = new.astype(BF)


def step(
    inputs,
    key_cot,
    value_cot,
    key_basis,
    value_basis,
    key_weight,
    value_weight,
    key_mean,
    key_var,
    value_mean,
    value_var,
):
    t = lax.axis_index("tp")
    planes = lax.axis_size(PLANE)
    tp_size = lax.axis_size("tp")
    devices = lax.axis_size(FS) * tp_size
    moments = (key_mean, key_var, value_mean, value_var)
    rank = key_basis.shape[1]
    width = (key_cot.shape[1] + value_cot.shape[1]) // 2
    two_rows = 2 * key_mean.shape[0]

    both = jnp.concatenate([key_basis, value_basis], axis=1)
    quarter = both.shape[1] // tp_size
    own = spread(lax.dynamic_slice_in_dim(both, t * quarter, quarter, axis=1), PLANE)
    other = other_core(own)
    tok = inputs.shape[0] // 2
    first, basis = mapped_kernel(inputs, 0, tok, quarter, own, other_core(own))
    last = mapped_kernel(inputs, tok, tok, quarter, basis)

    up = [(i, (i + 1) % tp_size) for i in range(tp_size)]
    down = [(i, (i - 1) % tp_size) for i in range(tp_size)]
    first_up = lax.ppermute(first, "tp", up)
    first_down = lax.ppermute(first, "tp", down)
    last_up = lax.ppermute(last, "tp", up)
    last_down = lax.ppermute(last, "tp", down)
    far_first = lax.ppermute(first_up, "tp", up)
    far_last = lax.ppermute(last_down, "tp", down)
    blocks = (first, last, first_down, last_down, far_first, far_last, first_up, last_up)

    flops = 2 * rank * inputs.shape[0] * width
    mapped, theirs = local(
        part_theirs_body, (shape((2 * rank, inputs.shape[0]), BF), shape((rank, width), BF)), flops
    )(*blocks, key_cot, value_cot)
    got = other_core(theirs)
    ours = local(part_ours_body, shape((rank, width)), flops)(mapped, key_cot, value_cot)
    pair = (ours + got.astype(F32)).astype(BF)

    beside = [(i, i ^ 1) for i in range(tp_size)]
    across = [(i, tp_size - 1 - i) for i in range(tp_size)]
    basis, _ = lax.optimization_barrier((basis, mapped))
    basis_y = lax.ppermute(basis, "tp", beside)

    stat = shape((two_rows, width))
    held = (key_basis, value_basis, key_weight, value_weight)
    mine, theirs, key_rows, value_rows, key_old, value_old = local(
        stats_body, (stat, stat) + tuple(shape(a.shape, a.dtype) for a in held)
    )(*moments, *held)
    stats = other_core(theirs)
    arrived = lax.all_to_all(pair.reshape(planes, -1, width), PLANE, 0, 0, tiled=True)
    dirs, own_new, back = local(
        moments_body, (shape(arrived.shape, BF), stat, stat)
    )(arrived, mine, stats)
    own_dir = lax.all_to_all(dirs, PLANE, 0, 0, tiled=True).reshape(rank, width)

    gram = local(gram_body, shape((rank, rank)), 4 * basis.size * rank)(basis, basis_y)
    gram_y = lax.ppermute(gram, "tp", across)
    new_moments = local(placed_body, tuple(shape(a.shape) for a in moments))(
        own_new, other_core(back)
    )

    key_up, value_up, sums = local(
        update_body,
        (shape(key_weight.shape), shape(value_weight.shape), shape((1, 128))),
        8 * rank * rank * width,
    )(own_dir, other_core(own_dir), key_rows, value_rows, gram, gram_y)
    sums = [sums] + [
        lax.ppermute(sums, "tp", [(i, (i + k) % tp_size) for i in range(tp_size)])
        for k in range(1, tp_size)
    ]
    counts = (float(key_weight.size * devices), float(value_weight.size * devices))
    key_new, value_new, key_copy, value_copy = local(
        functools.partial(finish_body, counts),
        (
            shape(key_weight.shape),
            shape(value_weight.shape),
            shape(key_weight.shape, BF),
            shape(value_weight.shape, BF),
        ),
    )(*sums, key_up, value_up, key_old, value_old)
    key_mean_new, key_var_new, value_mean_new, value_var_new = new_moments
    return (
        key_new,
        value_new,
        key_copy,
        value_copy,
        key_mean_new,
        key_var_new,
        value_mean_new,
        value_var_new,
    )


def solution(mesh):
    split = Mesh(mesh.devices.reshape(8, 4, 2, mesh.shape["tp"]), ("z", "x", "c", "tp"))
    rows, tiles = P(FS, None), P(FS, "tp")
    return jax.shard_map(
        step,
        mesh=split,
        in_specs=(rows, tiles, tiles, rows, rows) + (tiles,) * 6,
        out_specs=(tiles,) * 8,
        check_vma=False,
    )
```

```python
import functools

import jax
import jax.numpy as jnp
from jax import lax
from jax.experimental import pallas as pl
from jax.experimental.pallas import tpu as pltpu
from jax.sharding import Mesh
from jax.sharding import PartitionSpec as P


FS = ("z", "x", "c")
PLANE = ("z", "x")
SWAP = [(0, 1), (1, 0)]
BF = jnp.bfloat16
F32 = jnp.float32
VMEM = pl.BlockSpec(memory_space=pltpu.VMEM)


def spread(shard, axes):
    peers = lax.axis_size(axes)
    return lax.all_to_all(
        jnp.broadcast_to(shard[None], (peers, *shard.shape)), axes, 0, 0, tiled=True
    )


def other_core(a):
    return lax.ppermute(a, "c", SWAP)


def shape(dims, dtype=F32):
    return jax.ShapeDtypeStruct(dims, dtype)


def local(body, outs, flops=0, mib=16):
    def call(*arrays):
        return pl.pallas_call(
            body,
            out_shape=outs,
            in_specs=[VMEM] * len(arrays),
            out_specs=(VMEM,) * len(outs) if isinstance(outs, tuple) else VMEM,
            compiler_params=pltpu.CompilerParams(vmem_limit_bytes=mib << 20),
            cost_estimate=pl.CostEstimate(
                flops=max(flops, 1 << 20), bytes_accessed=1 << 20, transcendentals=0
            ),
        )(*arrays)

    return call


def mapped_body(fresh, *refs):
    if fresh:
        x_ref, own_ref, other_ref, out_ref, basis = refs
        c, x = lax.axis_index("c"), lax.axis_index("x")
        peers = own_ref.shape[0]
        for away in range(peers):
            at = lax.rem(x + away, peers)
            basis[:, at, c] = own_ref[away]
            basis[:, at, 1 - c] = other_ref[away]
    else:
        x_ref, basis, out_ref = refs
    whole = basis[...].reshape(x_ref.shape[1], -1)
    out_ref[...] = jnp.dot(x_ref[...], whole, preferred_element_type=F32).T.astype(BF)


def mapped_kernel(x, *factor):
    tok, depth = x.shape
    quarter = factor[0].shape[-1]
    fresh = len(factor) == 2
    out = shape((quarter, tok), BF)
    peers, far, rows = factor[0].shape[:3]
    return local(
        functools.partial(mapped_body, fresh),
        (out, shape((far, peers, 2, rows, quarter), BF)) if fresh else out,
        4 * tok * depth * quarter,
    )(x, *factor)


def part_half(side, m_ref, k_ref, v_ref, out_ref):
    rank = m_ref.shape[0] // 2
    kw, vw = k_ref.shape[1] // 2, v_ref.shape[1] // 2
    kc = k_ref[:, pl.ds(pl.multiple_of(side * kw, 128), kw)]
    vc = v_ref[:, pl.ds(pl.multiple_of(side * vw, 128), vw)]
    out_ref[:, :kw] = jnp.dot(m_ref[:rank], kc, preferred_element_type=F32).astype(out_ref.dtype)
    out_ref[:, kw:] = jnp.dot(m_ref[rank:], vc, preferred_element_type=F32).astype(out_ref.dtype)


def part_theirs_body(*refs):
    blocks, (k_ref, v_ref, m_ref, out_ref) = refs[:-4], refs[-4:]
    t = lax.axis_index("tp")
    quarter, tok = blocks[0].shape
    peers = len(blocks) // 2
    for away in range(peers):
        rows = pl.ds(pl.multiple_of(lax.rem(t + away, peers) * quarter, quarter), quarter)
        m_ref[rows, :tok] = blocks[2 * away][...]
        m_ref[rows, tok:] = blocks[2 * away + 1][...]
    part_half(1 - lax.axis_index("c"), m_ref, k_ref, v_ref, out_ref)


def part_ours_body(m_ref, k_ref, v_ref, out_ref):
    part_half(lax.axis_index("c"), m_ref, k_ref, v_ref, out_ref)


def stats_body(km, kv, vm, vv, *refs):
    held, (mine, theirs), staged = refs[:4], refs[4:6], refs[6:]
    c = lax.axis_index("c")
    rows = km.shape[0]
    kw, vw = km.shape[1] // 2, vm.shape[1] // 2
    for out, side in ((mine, c), (theirs, 1 - c)):
        ks, vs = (pl.ds(pl.multiple_of(side * w, 128), w) for w in (kw, vw))
        out[:rows, :kw] = km[:, ks]
        out[:rows, kw:] = vm[:, vs]
        out[rows:, :kw] = kv[:, ks]
        out[rows:, kw:] = vv[:, vs]
    for src, dst in zip(held, staged):
        dst[...] = src[...]


def moments_body(arrived, mine, theirs, dirs, own_new, back):
    first = lax.axis_index("c") == 0
    rows = mine.shape[0] // 2
    proj = jnp.sum(arrived[...].astype(F32), axis=0)

    def both(at):
        own, other = mine[at : at + rows], theirs[at : at + rows]
        low = jnp.where(first, own, other)
        high = jnp.where(first, other, own)
        return jnp.concatenate([low, high], axis=0)

    mean_new = 0.8 * both(0) + 0.2 * proj
    var_new = 0.9 * both(rows) + 0.1 * proj * proj
    d = (mean_new / (jnp.sqrt(var_new) + 1e-08)).astype(BF)
    dirs[...] = jnp.broadcast_to(d[None], dirs.shape)
    for at, new in ((0, mean_new), (rows, var_new)):
        low, high = new[:rows], new[rows:]
        own_new[at : at + rows] = jnp.where(first, low, high)
        back[at : at + rows] = jnp.where(first, high, low)


def placed_body(own, back, km, kv, vm, vv):
    c = lax.axis_index("c")
    rows = km.shape[0]
    kw, vw = km.shape[1] // 2, vm.shape[1] // 2
    for src, side in ((own, c), (back, 1 - c)):
        ks, vs = (pl.ds(pl.multiple_of(side * w, 128), w) for w in (kw, vw))
        km[:, ks] = src[:rows, :kw]
        vm[:, vs] = src[:rows, kw:]
        kv[:, ks] = src[rows:, :kw]
        vv[:, vs] = src[rows:, kw:]


def gram_body(mine, beside, out):
    first = lax.axis_index("tp") % 2 == 0
    low = jnp.where(first, mine[...], beside[...])
    high = jnp.where(first, beside[...], mine[...])
    cols = jnp.concatenate([low, high], axis=1)
    out[...] = lax.dot_general(
        cols, cols, (((0,), (0,)), ((), ())), preferred_element_type=F32
    )


def update_body(own, other, kb, vb, gram, gram_y, key_up, value_up, sums):
    c, t = lax.axis_index("c"), lax.axis_index("tp")
    kw, vw = key_up.shape[1] // 2, value_up.shape[1] // 2
    is_key = t < 2
    key_gram = jnp.where(is_key, gram[...], gram_y[...])
    value_gram = jnp.where(is_key, gram_y[...], gram[...])

    def pieces(g):
        a = g.astype(BF)
        r = g - a.astype(F32)
        b = r.astype(BF)
        return a, b, (r - b.astype(F32)).astype(BF)

    def square(ps, d):
        gd = sum(jnp.dot(p, d, preferred_element_type=F32) for p in ps)
        return jnp.sum(gd * d.astype(F32), axis=0, keepdims=True)

    kp, vp = pieces(key_gram), pieces(value_gram)
    ksq = jnp.zeros((1, kw), F32)
    vsq = jnp.zeros((1, vw), F32)
    for src, side in ((own, c), (other, 1 - c)):
        dk, dv = src[:, :kw], src[:, kw:]
        ks, vs = (pl.ds(pl.multiple_of(side * w, 128), w) for w in (kw, vw))
        key_up[:, ks] = jnp.dot(kb[...], dk, preferred_element_type=F32)
        value_up[:, vs] = jnp.dot(vb[...], dv, preferred_element_type=F32)
        ksq += square(kp, dk)
        vsq += square(vp, dv)
    lane = lax.broadcasted_iota(jnp.int32, sums.shape, 1)
    sums[...] = jnp.where(lane == 0, jnp.sum(ksq), jnp.where(lane == 1, jnp.sum(vsq), 0.0))


def finish_body(counts, s0, s1, s2, s3, ku, vu, kw, vw, kn, vn, kc, vc):
    total = (s0[...] + s1[...]) + (s2[...] + s3[...])
    for lane, u, w, n, b in ((0, ku, kw, kn, kc), (1, vu, vw, vn, vc)):
        mean = total[:, lane : lane + 1] / counts[lane]
        factor = jnp.minimum(1.0, 0.5 * lax.rsqrt(mean + 1e-06))
        new = w[...] - 0.25 * factor * u[...]
        n[...] = new
        b[...] = new.astype(BF)


def step(
    inputs,
    key_cot,
    value_cot,
    key_basis,
    value_basis,
    key_weight,
    value_weight,
    key_mean,
    key_var,
    value_mean,
    value_var,
):
    t = lax.axis_index("tp")
    planes = lax.axis_size(PLANE)
    tp_size = lax.axis_size("tp")
    devices = lax.axis_size(FS) * tp_size
    moments = (key_mean, key_var, value_mean, value_var)
    rank = key_basis.shape[1]
    width = (key_cot.shape[1] + value_cot.shape[1]) // 2
    two_rows = 2 * key_mean.shape[0]

    both = jnp.concatenate([key_basis, value_basis], axis=1)
    quarter = both.shape[1] // tp_size
    tok = inputs.shape[0] // 2
    shard = lax.dynamic_slice_in_dim(both, t * quarter, quarter, axis=1)
    near = spread(shard, "z")
    x_size = lax.axis_size("x")
    own = [near]
    for away in range(1, x_size):
        own.append(
            lax.ppermute(near, "x", [((i + away) % x_size, i) for i in range(x_size)])
        )
    own = jnp.stack(own)
    x_first, x_last = inputs[:tok], inputs[tok:]
    first, basis = mapped_kernel(x_first, own, other_core(own))
    last = mapped_kernel(x_last, basis)

    up = [(i, (i + 1) % tp_size) for i in range(tp_size)]
    down = [(i, (i - 1) % tp_size) for i in range(tp_size)]
    first_up = lax.ppermute(first, "tp", up)
    first_down = lax.ppermute(first, "tp", down)
    last_up = lax.ppermute(last, "tp", up)
    last_down = lax.ppermute(last, "tp", down)
    far_first = lax.ppermute(first_up, "tp", up)
    far_last = lax.ppermute(last_down, "tp", down)
    blocks = (first, last, first_down, last_down, far_first, far_last, first_up, last_up)

    flops = 2 * rank * inputs.shape[0] * width
    mapped, theirs = local(
        part_theirs_body, (shape((2 * rank, inputs.shape[0]), BF), shape((rank, width), BF)), flops
    )(*blocks, key_cot, value_cot)
    got = other_core(theirs)
    ours = local(part_ours_body, shape((rank, width)), flops)(mapped, key_cot, value_cot)
    pair = (ours + got.astype(F32)).astype(BF)

    beside = [(i, i ^ 1) for i in range(tp_size)]
    across = [(i, tp_size - 1 - i) for i in range(tp_size)]
    basis_y = lax.ppermute(basis, "tp", beside)

    stat = shape((two_rows, width))
    held = (key_basis, value_basis, key_weight, value_weight)
    mine, theirs, key_rows, value_rows, key_old, value_old = local(
        stats_body, (stat, stat) + tuple(shape(a.shape, a.dtype) for a in held)
    )(*moments, *held)
    stats = other_core(theirs)
    arrived = lax.all_to_all(pair.reshape(planes, -1, width), PLANE, 0, 0, tiled=True)
    dirs, own_new, back = local(
        moments_body, (shape(arrived.shape, BF), stat, stat)
    )(arrived, mine, stats)
    own_dir = lax.all_to_all(dirs, PLANE, 0, 0, tiled=True).reshape(rank, width)

    gram = local(gram_body, shape((rank, rank)), 4 * basis.size * rank)(
        basis.reshape(-1, quarter), basis_y.reshape(-1, quarter)
    )
    gram_y = lax.ppermute(gram, "tp", across)
    new_moments = local(placed_body, tuple(shape(a.shape) for a in moments))(
        own_new, other_core(back)
    )

    key_up, value_up, sums = local(
        update_body,
        (shape(key_weight.shape), shape(value_weight.shape), shape((1, 128))),
        8 * rank * rank * width,
    )(own_dir, other_core(own_dir), key_rows, value_rows, gram, gram_y)
    sums = [sums] + [
        lax.ppermute(sums, "tp", [(i, (i + k) % tp_size) for i in range(tp_size)])
        for k in range(1, tp_size)
    ]
    counts = (float(key_weight.size * devices), float(value_weight.size * devices))
    key_new, value_new, key_copy, value_copy = local(
        functools.partial(finish_body, counts),
        (
            shape(key_weight.shape),
            shape(value_weight.shape),
            shape(key_weight.shape, BF),
            shape(value_weight.shape, BF),
        ),
    )(*sums, key_up, value_up, key_old, value_old)
    key_mean_new, key_var_new, value_mean_new, value_var_new = new_moments
    return (
        key_new,
        value_new,
        key_copy,
        value_copy,
        key_mean_new,
        key_var_new,
        value_mean_new,
        value_var_new,
    )


def solution(mesh):
    split = Mesh(mesh.devices.reshape(8, 4, 2, mesh.shape["tp"]), ("z", "x", "c", "tp"))
    rows, tiles = P(FS, None), P(FS, "tp")
    return jax.shard_map(
        step,
        mesh=split,
        in_specs=(rows, tiles, tiles, rows, rows) + (tiles,) * 6,
        out_specs=(tiles,) * 8,
        check_vma=False,
    )
```

```python
import functools

import jax
import jax.numpy as jnp
from jax import lax
from jax.experimental import pallas as pl
from jax.experimental.pallas import tpu as pltpu
from jax.sharding import Mesh
from jax.sharding import PartitionSpec as P


FS = ("z", "x", "c")
PLANE = ("z", "x")
SWAP = [(0, 1), (1, 0)]
BF = jnp.bfloat16
FIRST = 512
F32 = jnp.float32
VMEM = pl.BlockSpec(memory_space=pltpu.VMEM)


def spread(shard, axes):
    peers = lax.axis_size(axes)
    return lax.all_to_all(
        jnp.broadcast_to(shard[None], (peers, *shard.shape)), axes, 0, 0, tiled=True
    )


def other_core(a):
    return lax.ppermute(a, "c", SWAP)


def shape(dims, dtype=F32):
    return jax.ShapeDtypeStruct(dims, dtype)


def local(body, outs, flops=0, mib=16):
    def call(*arrays):
        return pl.pallas_call(
            body,
            out_shape=outs,
            in_specs=[VMEM] * len(arrays),
            out_specs=(VMEM,) * len(outs) if isinstance(outs, tuple) else VMEM,
            compiler_params=pltpu.CompilerParams(vmem_limit_bytes=mib << 20),
            cost_estimate=pl.CostEstimate(
                flops=max(flops, 1 << 20), bytes_accessed=1 << 20, transcendentals=0
            ),
        )(*arrays)

    return call


def mapped_body(fresh, *refs):
    if fresh:
        x_ref, own_ref, other_ref, out_ref, basis = refs
        c, x = lax.axis_index("c"), lax.axis_index("x")
        peers = own_ref.shape[0]
        for away in range(peers):
            at = lax.rem(x + away, peers)
            basis[:, at, c] = own_ref[away]
            basis[:, at, 1 - c] = other_ref[away]
    else:
        x_ref, basis, out_ref = refs
    whole = basis[...].reshape(x_ref.shape[1], -1)
    out_ref[...] = jnp.dot(x_ref[...], whole, preferred_element_type=F32).T.astype(BF)


def mapped_kernel(x, *factor):
    tok, depth = x.shape
    quarter = factor[0].shape[-1]
    fresh = len(factor) == 2
    out = shape((quarter, tok), BF)
    peers, far, rows = factor[0].shape[:3]
    return local(
        functools.partial(mapped_body, fresh),
        (out, shape((far, peers, 2, rows, quarter), BF)) if fresh else out,
        4 * tok * depth * quarter,
    )(x, *factor)


def part_half(side, m_ref, k_ref, v_ref, out_ref):
    rank = m_ref.shape[0] // 2
    kw, vw = k_ref.shape[1] // 2, v_ref.shape[1] // 2
    kc = k_ref[:, pl.ds(pl.multiple_of(side * kw, 128), kw)]
    vc = v_ref[:, pl.ds(pl.multiple_of(side * vw, 128), vw)]
    out_ref[:, :kw] = jnp.dot(m_ref[:rank], kc, preferred_element_type=F32).astype(out_ref.dtype)
    out_ref[:, kw:] = jnp.dot(m_ref[rank:], vc, preferred_element_type=F32).astype(out_ref.dtype)


def part_theirs_body(*refs):
    blocks, (k_ref, v_ref, m_ref, out_ref) = refs[:-4], refs[-4:]
    t = lax.axis_index("tp")
    quarter, tok = blocks[0].shape
    peers = len(blocks) // 2
    for away in range(peers):
        rows = pl.ds(pl.multiple_of(lax.rem(t + away, peers) * quarter, quarter), quarter)
        m_ref[rows, :tok] = blocks[2 * away][...]
        m_ref[rows, tok:] = blocks[2 * away + 1][...]
    part_half(1 - lax.axis_index("c"), m_ref, k_ref, v_ref, out_ref)


def part_ours_body(m_ref, k_ref, v_ref, out_ref):
    part_half(lax.axis_index("c"), m_ref, k_ref, v_ref, out_ref)


def stats_body(km, kv, vm, vv, *refs):
    held, (mine, theirs), staged = refs[:4], refs[4:6], refs[6:]
    c = lax.axis_index("c")
    rows = km.shape[0]
    kw, vw = km.shape[1] // 2, vm.shape[1] // 2
    for out, side in ((mine, c), (theirs, 1 - c)):
        ks, vs = (pl.ds(pl.multiple_of(side * w, 128), w) for w in (kw, vw))
        out[:rows, :kw] = km[:, ks]
        out[:rows, kw:] = vm[:, vs]
        out[rows:, :kw] = kv[:, ks]
        out[rows:, kw:] = vv[:, vs]
    for src, dst in zip(held, staged):
        dst[...] = src[...]


def moments_body(arrived, mine, theirs, dirs, own_new, back):
    first = lax.axis_index("c") == 0
    rows = mine.shape[0] // 2
    proj = jnp.sum(arrived[...].astype(F32), axis=0)

    def both(at):
        own, other = mine[at : at + rows], theirs[at : at + rows]
        low = jnp.where(first, own, other)
        high = jnp.where(first, other, own)
        return jnp.concatenate([low, high], axis=0)

    mean_new = 0.8 * both(0) + 0.2 * proj
    var_new = 0.9 * both(rows) + 0.1 * proj * proj
    d = (mean_new / (jnp.sqrt(var_new) + 1e-08)).astype(BF)
    dirs[...] = jnp.broadcast_to(d[None], dirs.shape)
    for at, new in ((0, mean_new), (rows, var_new)):
        low, high = new[:rows], new[rows:]
        own_new[at : at + rows] = jnp.where(first, low, high)
        back[at : at + rows] = jnp.where(first, high, low)


def placed_body(own, back, km, kv, vm, vv):
    c = lax.axis_index("c")
    rows = km.shape[0]
    kw, vw = km.shape[1] // 2, vm.shape[1] // 2
    for src, side in ((own, c), (back, 1 - c)):
        ks, vs = (pl.ds(pl.multiple_of(side * w, 128), w) for w in (kw, vw))
        km[:, ks] = src[:rows, :kw]
        vm[:, vs] = src[:rows, kw:]
        kv[:, ks] = src[rows:, :kw]
        vv[:, vs] = src[rows:, kw:]


def gram_body(mine, beside, out):
    first = lax.axis_index("tp") % 2 == 0
    low = jnp.where(first, mine[...], beside[...])
    high = jnp.where(first, beside[...], mine[...])
    cols = jnp.concatenate([low, high], axis=1)
    out[...] = lax.dot_general(
        cols, cols, (((0,), (0,)), ((), ())), preferred_element_type=F32
    )


def update_body(d, kb, vb, key_up, value_up):
    kw = key_up.shape[1]
    key_up[...] = jnp.dot(kb[...], d[:, :kw], preferred_element_type=F32)
    value_up[...] = jnp.dot(vb[...], d[:, kw:], preferred_element_type=F32)


def square_body(d, gram, gram_y, *refs):
    before, sums = refs[:-1], refs[-1]
    kw = d.shape[1] // 3
    is_key = lax.axis_index("tp") < 2
    key_gram = jnp.where(is_key, gram[...], gram_y[...])
    value_gram = jnp.where(is_key, gram_y[...], gram[...])
    lane = lax.broadcasted_iota(jnp.int32, sums.shape, 1)
    total = sum((ref[...] for ref in before), jnp.zeros(sums.shape, F32))
    for at, g, cols in ((0, key_gram, d[:, :kw]), (1, value_gram, d[:, kw:])):
        dd = lax.dot_general(
            cols, cols, (((1,), (1,)), ((), ())), preferred_element_type=F32
        )
        total += jnp.where(lane == at, jnp.sum(g * dd), 0.0)
    sums[...] = total


def finish_body(counts, s0, s1, s2, s3, ku, ku_far, vu, vu_far, kw, vw, kn, vn, kc, vc):
    c = lax.axis_index("c")
    total = (s0[...] + s1[...]) + (s2[...] + s3[...])
    for lane, ups, w, n, b in ((0, (ku, ku_far), kw, kn, kc), (1, (vu, vu_far), vw, vn, vc)):
        mean = total[:, lane : lane + 1] / counts[lane]
        factor = jnp.minimum(1.0, 0.5 * lax.rsqrt(mean + 1e-06))
        for u, side in zip(ups, (c, 1 - c)):
            width = u.shape[1]
            at = pl.ds(pl.multiple_of(side * width, 128), width)
            new = w[:, at] - 0.25 * factor * u[...]
            n[:, at] = new
            b[:, at] = new.astype(BF)


def step(
    inputs,
    key_cot,
    value_cot,
    key_basis,
    value_basis,
    key_weight,
    value_weight,
    key_mean,
    key_var,
    value_mean,
    value_var,
):
    t = lax.axis_index("tp")
    planes = lax.axis_size(PLANE)
    tp_size = lax.axis_size("tp")
    devices = lax.axis_size(FS) * tp_size
    moments = (key_mean, key_var, value_mean, value_var)
    rank = key_basis.shape[1]
    width = (key_cot.shape[1] + value_cot.shape[1]) // 2
    two_rows = 2 * key_mean.shape[0]

    both = jnp.concatenate([key_basis, value_basis], axis=1)
    quarter = both.shape[1] // tp_size
    tok = FIRST
    shard = lax.dynamic_slice_in_dim(both, t * quarter, quarter, axis=1)
    near = spread(shard, "z")
    x_size = lax.axis_size("x")
    own = [near]
    for away in range(1, x_size):
        own.append(
            lax.ppermute(near, "x", [((i + away) % x_size, i) for i in range(x_size)])
        )
    own = jnp.stack(own)
    x_first, x_last = inputs[:tok], inputs[tok:]
    first, basis = mapped_kernel(x_first, own, other_core(own))
    last = mapped_kernel(x_last, basis)

    up = [(i, (i + 1) % tp_size) for i in range(tp_size)]
    down = [(i, (i - 1) % tp_size) for i in range(tp_size)]
    first_up = lax.ppermute(first, "tp", up)
    first_down = lax.ppermute(first, "tp", down)
    last_up = lax.ppermute(last, "tp", up)
    last_down = lax.ppermute(last, "tp", down)
    far_first = lax.ppermute(first_up, "tp", up)
    far_last = lax.ppermute(last_down, "tp", down)
    blocks = (first, last, first_down, last_down, far_first, far_last, first_up, last_up)

    flops = 2 * rank * inputs.shape[0] * width
    mapped, theirs = local(
        part_theirs_body, (shape((2 * rank, inputs.shape[0]), BF), shape((rank, width), BF)), flops
    )(*blocks, key_cot, value_cot)
    got = other_core(theirs)
    ours = local(part_ours_body, shape((rank, width)), flops)(mapped, key_cot, value_cot)
    pair = (ours + got.astype(F32)).astype(BF)

    beside = [(i, i ^ 1) for i in range(tp_size)]
    across = [(i, tp_size - 1 - i) for i in range(tp_size)]
    basis_y = lax.ppermute(basis, "tp", beside)

    stat = shape((two_rows, width))
    held = (key_basis, value_basis, key_weight, value_weight)
    mine, theirs, key_rows, value_rows, key_old, value_old = local(
        stats_body, (stat, stat) + tuple(shape(a.shape, a.dtype) for a in held)
    )(*moments, *held)
    stats = other_core(theirs)
    arrived = lax.all_to_all(pair.reshape(planes, -1, width), PLANE, 0, 0, tiled=True)
    dirs, own_new, back = local(
        moments_body, (shape(arrived.shape, BF), stat, stat)
    )(arrived, mine, stats)
    own_dir = lax.all_to_all(dirs, PLANE, 0, 0, tiled=True).reshape(rank, width)

    gram = local(gram_body, shape((rank, rank)), 4 * basis.size * rank)(
        basis.reshape(-1, quarter), basis_y.reshape(-1, quarter)
    )
    gram_y = lax.ppermute(gram, "tp", across)
    new_moments = local(placed_body, tuple(shape(a.shape) for a in moments))(
        own_new, other_core(back)
    )

    far_dir = other_core(own_dir)
    sums = ()
    for d in (own_dir, far_dir):
        sums = local(square_body, shape((1, 128)), 4 * rank * rank * width)(d, gram, gram_y, *sums)
        sums = (sums,)
    (sums,) = sums
    parts = [sums]
    for away in range(1, tp_size):
        parts.append(lax.ppermute(sums, "tp", [(i, (i + away) % tp_size) for i in range(tp_size)]))
    sums = parts
    ups = tuple(shape((a.shape[0], a.shape[1] // 2)) for a in (key_weight, value_weight))
    key_up, value_up = zip(
        *(local(update_body, ups)(d, key_rows, value_rows) for d in (own_dir, far_dir))
    )
    counts = (float(key_weight.size * devices), float(value_weight.size * devices))
    key_new, value_new, key_copy, value_copy = local(
        functools.partial(finish_body, counts),
        (
            shape(key_weight.shape),
            shape(value_weight.shape),
            shape(key_weight.shape, BF),
            shape(value_weight.shape, BF),
        ),
    )(*sums, *key_up, *value_up, key_old, value_old)
    key_mean_new, key_var_new, value_mean_new, value_var_new = new_moments
    return (
        key_new,
        value_new,
        key_copy,
        value_copy,
        key_mean_new,
        key_var_new,
        value_mean_new,
        value_var_new,
    )


def solution(mesh):
    split = Mesh(mesh.devices.reshape(8, 4, 2, mesh.shape["tp"]), ("z", "x", "c", "tp"))
    rows, tiles = P(FS, None), P(FS, "tp")
    return jax.shard_map(
        step,
        mesh=split,
        in_specs=(rows, tiles, tiles, rows, rows) + (tiles,) * 6,
        out_specs=(tiles,) * 8,
        check_vma=False,
    )
```

```python
import functools

import jax
import jax.numpy as jnp
from jax import lax
from jax.experimental import pallas as pl
from jax.experimental.pallas import tpu as pltpu
from jax.sharding import Mesh
from jax.sharding import PartitionSpec as P


FS = ("z", "x", "c")
PLANE = ("z", "x")
SWAP = [(0, 1), (1, 0)]
BF = jnp.bfloat16
FIRST = 512
F32 = jnp.float32
VMEM = pl.BlockSpec(memory_space=pltpu.VMEM)


def spread(shard, axes):
    peers = lax.axis_size(axes)
    return lax.all_to_all(
        jnp.broadcast_to(shard[None], (peers, *shard.shape)), axes, 0, 0, tiled=True
    )


def other_core(a):
    return lax.ppermute(a, "c", SWAP)


def shape(dims, dtype=F32):
    return jax.ShapeDtypeStruct(dims, dtype)


def local(body, outs, flops=0, mib=16):
    def call(*arrays):
        return pl.pallas_call(
            body,
            out_shape=outs,
            in_specs=[VMEM] * len(arrays),
            out_specs=(VMEM,) * len(outs) if isinstance(outs, tuple) else VMEM,
            compiler_params=pltpu.CompilerParams(vmem_limit_bytes=mib << 20),
            cost_estimate=pl.CostEstimate(
                flops=max(flops, 1 << 20), bytes_accessed=1 << 20, transcendentals=0
            ),
        )(*arrays)

    return call


STRIP = 128


def staged_body(x_ref, *refs):
    outs, sems = refs[:-1], refs[-1]
    copies, at = [], 0
    for out in outs:
        for row in range(0, out.shape[0], STRIP):
            src = x_ref.at[pl.ds(at, STRIP)]
            copies.append(
                pltpu.make_async_copy(src, out.at[pl.ds(row, STRIP)], sems.at[len(copies)])
            )
            at += STRIP
    for copy in copies:
        copy.start()
    for copy in copies:
        copy.wait()


def staged(x, cuts):
    return pl.pallas_call(
        staged_body,
        out_shape=tuple(shape((rows, x.shape[1]), x.dtype) for rows in cuts),
        in_specs=[pl.BlockSpec(memory_space=pltpu.HBM)],
        out_specs=(VMEM,) * len(cuts),
        scratch_shapes=[pltpu.SemaphoreType.DMA((x.shape[0] // STRIP,))],
        name="staged",
        compiler_params=pltpu.CompilerParams(vmem_limit_bytes=44 << 20),
        cost_estimate=pl.CostEstimate(flops=1 << 22, bytes_accessed=2 * x.size, transcendentals=0),
    )(x)


def mapped_body(fresh, *refs):
    if fresh:
        x_ref, own_ref, other_ref, out_ref, basis = refs
        c, x = lax.axis_index("c"), lax.axis_index("x")
        peers = own_ref.shape[0]
        for away in range(peers):
            at = lax.rem(x + away, peers)
            basis[:, at, c] = own_ref[away]
            basis[:, at, 1 - c] = other_ref[away]
    else:
        x_ref, basis, out_ref = refs
    whole = basis[...].reshape(x_ref.shape[1], -1)
    out_ref[...] = jnp.dot(x_ref[...], whole, preferred_element_type=F32).T.astype(BF)


def mapped_kernel(x, *factor):
    tok, depth = x.shape
    quarter = factor[0].shape[-1]
    fresh = len(factor) == 2
    out = shape((quarter, tok), BF)
    peers, far, rows = factor[0].shape[:3]
    return local(
        functools.partial(mapped_body, fresh),
        (out, shape((far, peers, 2, rows, quarter), BF)) if fresh else out,
        4 * tok * depth * quarter,
    )(x, *factor)


def part_half(side, m_ref, k_ref, v_ref, out_ref):
    rank = m_ref.shape[0] // 2
    kw, vw = k_ref.shape[1] // 2, v_ref.shape[1] // 2
    kc = k_ref[:, pl.ds(pl.multiple_of(side * kw, 128), kw)]
    vc = v_ref[:, pl.ds(pl.multiple_of(side * vw, 128), vw)]
    out_ref[:, :kw] = jnp.dot(m_ref[:rank], kc, preferred_element_type=F32).astype(out_ref.dtype)
    out_ref[:, kw:] = jnp.dot(m_ref[rank:], vc, preferred_element_type=F32).astype(out_ref.dtype)


def part_theirs_body(*refs):
    blocks, (k_ref, v_ref, m_ref, out_ref) = refs[:-4], refs[-4:]
    t = lax.axis_index("tp")
    quarter, tok = blocks[0].shape
    peers = len(blocks) // 2
    for away in range(peers):
        rows = pl.ds(pl.multiple_of(lax.rem(t + away, peers) * quarter, quarter), quarter)
        m_ref[rows, :tok] = blocks[2 * away][...]
        m_ref[rows, tok:] = blocks[2 * away + 1][...]
    part_half(1 - lax.axis_index("c"), m_ref, k_ref, v_ref, out_ref)


def part_ours_body(m_ref, k_ref, v_ref, out_ref):
    part_half(lax.axis_index("c"), m_ref, k_ref, v_ref, out_ref)


def stats_body(km, kv, vm, vv, *refs):
    held, (mine, theirs), staged = refs[:4], refs[4:6], refs[6:]
    c = lax.axis_index("c")
    rows = km.shape[0]
    kw, vw = km.shape[1] // 2, vm.shape[1] // 2
    for out, side in ((mine, c), (theirs, 1 - c)):
        ks, vs = (pl.ds(pl.multiple_of(side * w, 128), w) for w in (kw, vw))
        out[:rows, :kw] = km[:, ks]
        out[:rows, kw:] = vm[:, vs]
        out[rows:, :kw] = kv[:, ks]
        out[rows:, kw:] = vv[:, vs]
    for src, dst in zip(held, staged):
        dst[...] = src[...]


def moments_body(arrived, mine, theirs, dirs, own_new, back):
    first = lax.axis_index("c") == 0
    rows = mine.shape[0] // 2
    proj = jnp.sum(arrived[...].astype(F32), axis=0)

    def both(at):
        own, other = mine[at : at + rows], theirs[at : at + rows]
        low = jnp.where(first, own, other)
        high = jnp.where(first, other, own)
        return jnp.concatenate([low, high], axis=0)

    mean_new = 0.8 * both(0) + 0.2 * proj
    var_new = 0.9 * both(rows) + 0.1 * proj * proj
    d = (mean_new / (jnp.sqrt(var_new) + 1e-08)).astype(BF)
    dirs[...] = jnp.broadcast_to(d[None], dirs.shape)
    for at, new in ((0, mean_new), (rows, var_new)):
        low, high = new[:rows], new[rows:]
        own_new[at : at + rows] = jnp.where(first, low, high)
        back[at : at + rows] = jnp.where(first, high, low)


def placed_body(own, back, km, kv, vm, vv):
    c = lax.axis_index("c")
    rows = km.shape[0]
    kw, vw = km.shape[1] // 2, vm.shape[1] // 2
    for src, side in ((own, c), (back, 1 - c)):
        ks, vs = (pl.ds(pl.multiple_of(side * w, 128), w) for w in (kw, vw))
        km[:, ks] = src[:rows, :kw]
        vm[:, vs] = src[:rows, kw:]
        kv[:, ks] = src[rows:, :kw]
        vv[:, vs] = src[rows:, kw:]


def gram_body(mine, beside, out):
    first = lax.axis_index("tp") % 2 == 0
    low = jnp.where(first, mine[...], beside[...])
    high = jnp.where(first, beside[...], mine[...])
    cols = jnp.concatenate([low, high], axis=1)
    out[...] = lax.dot_general(
        cols, cols, (((0,), (0,)), ((), ())), preferred_element_type=F32
    )


def update_body(d, kb, vb, key_up, value_up):
    kw = key_up.shape[1]
    key_up[...] = jnp.dot(kb[...], d[:, :kw], preferred_element_type=F32)
    value_up[...] = jnp.dot(vb[...], d[:, kw:], preferred_element_type=F32)


def square_body(d, gram, gram_y, *refs):
    before, sums = refs[:-1], refs[-1]
    kw = d.shape[1] // 3
    is_key = lax.axis_index("tp") < 2
    key_gram = jnp.where(is_key, gram[...], gram_y[...])
    value_gram = jnp.where(is_key, gram_y[...], gram[...])
    lane = lax.broadcasted_iota(jnp.int32, sums.shape, 1)
    total = sum((ref[...] for ref in before), jnp.zeros(sums.shape, F32))
    for at, g, cols in ((0, key_gram, d[:, :kw]), (1, value_gram, d[:, kw:])):
        dd = lax.dot_general(
            cols, cols, (((1,), (1,)), ((), ())), preferred_element_type=F32
        )
        total += jnp.where(lane == at, jnp.sum(g * dd), 0.0)
    sums[...] = total


def finish_body(counts, s0, s1, s2, s3, ku, ku_far, vu, vu_far, kw, vw, kn, vn, kc, vc):
    c = lax.axis_index("c")
    total = (s0[...] + s1[...]) + (s2[...] + s3[...])
    for lane, ups, w, n, b in ((0, (ku, ku_far), kw, kn, kc), (1, (vu, vu_far), vw, vn, vc)):
        mean = total[:, lane : lane + 1] / counts[lane]
        factor = jnp.minimum(1.0, 0.5 * lax.rsqrt(mean + 1e-06))
        for u, side in zip(ups, (c, 1 - c)):
            width = u.shape[1]
            at = pl.ds(pl.multiple_of(side * width, 128), width)
            new = w[:, at] - 0.25 * factor * u[...]
            n[:, at] = new
            b[:, at] = new.astype(BF)


def step(
    inputs,
    key_cot,
    value_cot,
    key_basis,
    value_basis,
    key_weight,
    value_weight,
    key_mean,
    key_var,
    value_mean,
    value_var,
):
    t = lax.axis_index("tp")
    planes = lax.axis_size(PLANE)
    tp_size = lax.axis_size("tp")
    devices = lax.axis_size(FS) * tp_size
    moments = (key_mean, key_var, value_mean, value_var)
    rank = key_basis.shape[1]
    width = (key_cot.shape[1] + value_cot.shape[1]) // 2
    two_rows = 2 * key_mean.shape[0]

    both = jnp.concatenate([key_basis, value_basis], axis=1)
    quarter = both.shape[1] // tp_size
    tok = FIRST
    shard = lax.dynamic_slice_in_dim(both, t * quarter, quarter, axis=1)
    near = spread(shard, "z")
    x_size = lax.axis_size("x")
    own = [near]
    for away in range(1, x_size):
        own.append(
            lax.ppermute(near, "x", [((i + away) % x_size, i) for i in range(x_size)])
        )
    own = jnp.stack(own)
    x_first, x_last = staged(inputs, (tok, inputs.shape[0] - tok))
    first, basis = mapped_kernel(x_first, own, other_core(own))
    last = mapped_kernel(x_last, basis)

    up = [(i, (i + 1) % tp_size) for i in range(tp_size)]
    down = [(i, (i - 1) % tp_size) for i in range(tp_size)]
    first_up = lax.ppermute(first, "tp", up)
    first_down = lax.ppermute(first, "tp", down)
    last_up = lax.ppermute(last, "tp", up)
    last_down = lax.ppermute(last, "tp", down)
    far_first = lax.ppermute(first_up, "tp", up)
    far_last = lax.ppermute(last_down, "tp", down)
    blocks = (first, last, first_down, last_down, far_first, far_last, first_up, last_up)

    flops = 2 * rank * inputs.shape[0] * width
    mapped, theirs = local(
        part_theirs_body, (shape((2 * rank, inputs.shape[0]), BF), shape((rank, width), BF)), flops
    )(*blocks, key_cot, value_cot)
    got = other_core(theirs)
    ours = local(part_ours_body, shape((rank, width)), flops)(mapped, key_cot, value_cot)
    pair = (ours + got.astype(F32)).astype(BF)

    beside = [(i, i ^ 1) for i in range(tp_size)]
    across = [(i, tp_size - 1 - i) for i in range(tp_size)]
    basis_y = lax.ppermute(basis, "tp", beside)

    stat = shape((two_rows, width))
    held = (key_basis, value_basis, key_weight, value_weight)
    mine, theirs, key_rows, value_rows, key_old, value_old = local(
        stats_body, (stat, stat) + tuple(shape(a.shape, a.dtype) for a in held)
    )(*moments, *held)
    stats = other_core(theirs)
    arrived = lax.all_to_all(pair.reshape(planes, -1, width), PLANE, 0, 0, tiled=True)
    dirs, own_new, back = local(
        moments_body, (shape(arrived.shape, BF), stat, stat)
    )(arrived, mine, stats)
    own_dir = lax.all_to_all(dirs, PLANE, 0, 0, tiled=True).reshape(rank, width)

    gram = local(gram_body, shape((rank, rank)), 4 * basis.size * rank)(
        basis.reshape(-1, quarter), basis_y.reshape(-1, quarter)
    )
    gram_y = lax.ppermute(gram, "tp", across)
    new_moments = local(placed_body, tuple(shape(a.shape) for a in moments))(
        own_new, other_core(back)
    )

    far_dir = other_core(own_dir)
    sums = ()
    for d in (own_dir, far_dir):
        sums = local(square_body, shape((1, 128)), 4 * rank * rank * width)(d, gram, gram_y, *sums)
        sums = (sums,)
    (sums,) = sums
    parts = [sums]
    for away in range(1, tp_size):
        parts.append(lax.ppermute(sums, "tp", [(i, (i + away) % tp_size) for i in range(tp_size)]))
    sums = parts
    ups = tuple(shape((a.shape[0], a.shape[1] // 2)) for a in (key_weight, value_weight))
    key_up, value_up = zip(
        *(local(update_body, ups)(d, key_rows, value_rows) for d in (own_dir, far_dir))
    )
    counts = (float(key_weight.size * devices), float(value_weight.size * devices))
    key_new, value_new, key_copy, value_copy = local(
        functools.partial(finish_body, counts),
        (
            shape(key_weight.shape),
            shape(value_weight.shape),
            shape(key_weight.shape, BF),
            shape(value_weight.shape, BF),
        ),
    )(*sums, *key_up, *value_up, key_old, value_old)
    key_mean_new, key_var_new, value_mean_new, value_var_new = new_moments
    return (
        key_new,
        value_new,
        key_copy,
        value_copy,
        key_mean_new,
        key_var_new,
        value_mean_new,
        value_var_new,
    )


def solution(mesh):
    split = Mesh(mesh.devices.reshape(8, 4, 2, mesh.shape["tp"]), ("z", "x", "c", "tp"))
    rows, tiles = P(FS, None), P(FS, "tp")
    return jax.shard_map(
        step,
        mesh=split,
        in_specs=(rows, tiles, tiles, rows, rows) + (tiles,) * 6,
        out_specs=(tiles,) * 8,
        check_vma=False,
    )
```
